32 devices in a mesh: sp: 8 (over z, y), tp: 4 (over x, core).
Axes of the slice: x: 2, y: 2, z: 4, core: 2. Of those that a mesh axis runs over, the one named last changes fastest.
Arguments:
- tokens: bfloat16 [8192, 2048], P('sp', 'tp'), may hold values from -16 to 16
- mix_gain: float32 [2048], replicated, may hold values from 0.1 to 1.9
- query_weight: bfloat16 [2048, 1024], P(None, 'tp'), may hold values from -0.125 to 0.125
- key_weight: bfloat16 [2048, 1024], P(None, 'tp'), may hold values from -0.125 to 0.125
- value_weight: bfloat16 [2048, 1024], P(None, 'tp'), may hold values from -0.125 to 0.125
- outer_gate_weight: bfloat16 [2048, 1024], P(None, 'tp'), may hold values from -0.125 to 0.125
- inner_gate_weight: bfloat16 [2048, 1024], P(None, 'tp'), may hold values from -0.125 to 0.125
- conv_input_weight: bfloat16 [2048, 1024], P(None, 'tp'), may hold values from -0.125 to 0.125
- query_gain: float32 [64], replicated, may hold values from 0.6 to 10
- key_gain: float32 [64], replicated, may hold values from 0.6 to 10
- gate_totals: float32 [8192, 16], P('sp', 'tp'), may hold values from -2048 to 0, as said below
- conv_taps: float32 [3, 1024], P(None, 'tp'), may hold values from -3 to 3
- attn_out_gain: float32 [1024], P('tp'), may hold values from 0.1 to 1.9
- conv_out_gain: float32 [1024], P('tp'), may hold values from 0.1 to 1.9
- attn_out_weight: bfloat16 [1024, 2048], P('tp'), may hold values from -0.125 to 0.125
- conv_out_weight: bfloat16 [1024, 2048], P('tp'), may hold values from -0.125 to 0.125
Outputs:
- mixed: bfloat16 [8192, 2048], P(('sp', 'tp'))
The draws below stay inside these ranges and needn't reach their ends.
Inputs may be any that keep to these rules, and one draw needn't show every extreme that they name: `gate_totals`: in every head the values never rise from one position to the next.
All inputs are finite; a program needn't handle non-finite values.
Results may differ from the reference program's by a relative error of at most 0.015.
The reference program's roundings to bfloat16 on the way count: a program that leaves them out, or rounds other values in their place, can miss the bound.
Values may be sent and summed in bfloat16 or wider, within the bound.
No kernel may reach another device: no remote copies, remote signals or barrier semaphores. Data moves between devices by JAX's collectives and lax.ppermute only.
A program may use at most 64 MiB of HBM per device.

```python
import math
import jax
import jax.numpy as jnp
from jax import lax

D = 2048
HEAD_DIM = 64
ATTENTION_HEADS = 16
CONV_K = 3
TOK_DEV = 1024
ATTN_WIDTH = 1024
CONV_WIDTH = 1024
SEQUENCE_TOKENS = 8192
N_TP = 4


def draw_tokens(key, part):
    random_subkeys = jax.random.split(jax.random.fold_in(key, 101), 2)
    column = jnp.arange(D, dtype=jnp.float32) / D
    column_scale = 0.5 * jnp.exp(math.log(4.0) * column) * jax.random.uniform(random_subkeys[1], (D,), jnp.float32, 0.7, 1.4)
    normal_part = jax.random.normal(random_subkeys[0], (SEQUENCE_TOKENS, D), jnp.float32)
    return jnp.clip(normal_part * column_scale, -16.0, 16.0).astype(jnp.bfloat16)


def focus_gain(key):
    gain = jax.random.uniform(key, (HEAD_DIM,), jnp.float32, 0.6, 1.4)
    return gain


def draw_query_gain(key, part):
    return focus_gain(jax.random.fold_in(key, 211))


def draw_key_gain(key, part):
    return focus_gain(jax.random.fold_in(key, 307))


def draw_gate_totals(key, part):
    random_subkeys = jax.random.split(jax.random.fold_in(key, 401), 7)
    order = jax.random.permutation(random_subkeys[0], ATTENTION_HEADS)
    fast_path = order < ATTENTION_HEADS // 2
    slow_total = jax.random.uniform(random_subkeys[1], (ATTENTION_HEADS,), jnp.float32, 0.15, 0.5)
    quick_reach = jnp.exp(jax.random.uniform(random_subkeys[2], (ATTENTION_HEADS,), jnp.float32, math.log(30.0), math.log(100.0)))
    base_rate = jnp.where(fast_path, 1.0 / quick_reach, slow_total / SEQUENCE_TOKENS)
    block_factor = jnp.exp(jax.random.uniform(random_subkeys[3], (SEQUENCE_TOKENS // TOK_DEV, 1), jnp.float32, math.log(0.5), math.log(2.0)))
    block_rate = jnp.repeat(block_factor, TOK_DEV, axis=0)
    jitter = jnp.exp(jax.random.uniform(random_subkeys[4], (SEQUENCE_TOKENS, ATTENTION_HEADS), jnp.float32, math.log(0.5), math.log(2.0)))
    per_step_loss = base_rate[None, :] * block_rate * jitter
    spike_position = jax.random.randint(random_subkeys[5], (2,), 0, SEQUENCE_TOKENS)
    spike_hit = jnp.any(jnp.arange(SEQUENCE_TOKENS)[:, None] == spike_position[None, :], axis=1)
    spike_loss = jax.random.uniform(random_subkeys[6], (SEQUENCE_TOKENS, ATTENTION_HEADS), jnp.float32, 0.22, 0.51)
    per_step_loss = per_step_loss + jnp.where(spike_hit[:, None] & jnp.logical_not(fast_path)[None, :], spike_loss, 0.0)
    return -jnp.cumsum(per_step_loss, axis=0)


def block_levels(stream_key, shape, cuts, low, top_value):
    level, own = 1.0, jax.random.fold_in(stream_key, 6)
    for position, shards_of in cuts:
        draws = jnp.exp(jax.random.uniform(jax.random.fold_in(own, position), (shards_of,), jnp.float32, low / len(cuts), top_value / len(cuts)))
        level = level * jnp.repeat(draws, shape[position] // shards_of).reshape([-1 if axis == position else 1 for axis in range(len(shape))])
    return level


def centred(stream_key, shape, deviation, most, cuts=(), kind=jnp.bfloat16):
    array = deviation * jax.random.normal(stream_key, shape, jnp.float32)
    if cuts:
        array = array * block_levels(stream_key, shape, cuts, -0.22, 0.18)
    return jnp.clip(array, -most, most).astype(kind)


def setup_inputs(seed: int = 0) -> dict:
    key_of = jax.random.split(jax.random.key(seed), 17)
    return {
        "tokens": draw_tokens(jax.random.fold_in(key_of[16], 71), 0),
        "mix_gain": jnp.clip(1.0 + 0.18 * jax.random.normal(key_of[1], (D,), jnp.float32), 0.1, 1.9),
        "query_weight": centred(key_of[2], (D, ATTN_WIDTH), D ** -0.5, 0.125, ((1, 4),)),
        "key_weight": centred(key_of[3], (D, ATTN_WIDTH), D ** -0.5, 0.125, ((1, 4),)),
        "value_weight": centred(key_of[4], (D, ATTN_WIDTH), D ** -0.5, 0.125, ((1, 4),)),
        "outer_gate_weight": centred(key_of[5], (D, CONV_WIDTH), D ** -0.5, 0.125, ((1, 4),)),
        "inner_gate_weight": centred(key_of[6], (D, CONV_WIDTH), D ** -0.5, 0.125, ((1, 4),)),
        "conv_input_weight": centred(key_of[7], (D, CONV_WIDTH), D ** -0.5, 0.125, ((1, 4),)),
        "query_gain": draw_query_gain(jax.random.fold_in(key_of[16], 71), 0),
        "key_gain": draw_key_gain(jax.random.fold_in(key_of[16], 71), 0),
        "gate_totals": draw_gate_totals(jax.random.fold_in(key_of[16], 71), 0),
        "conv_taps": centred(key_of[11], (CONV_K, CONV_WIDTH), 0.6, 3.0, ((1, 4),), jnp.float32),
        "attn_out_gain": jnp.clip(1.0 + 0.18 * jax.random.normal(key_of[12], (ATTN_WIDTH,), jnp.float32), 0.1, 1.9),
        "conv_out_gain": jnp.clip(1.0 + 0.18 * jax.random.normal(key_of[13], (CONV_WIDTH,), jnp.float32), 0.1, 1.9),
        "attn_out_weight": centred(key_of[14], (ATTN_WIDTH, D), (ATTN_WIDTH + CONV_WIDTH) ** -0.5, 0.125, ((0, 4),)),
        "conv_out_weight": centred(key_of[15], (CONV_WIDTH, D), (ATTN_WIDTH + CONV_WIDTH) ** -0.5, 0.125, ((0, 4),)),
    }


NORM_EPSILON = 1e-06

def head_norm(values, head_dim, gain):
    row_count = values.shape[0]
    grouped = values.reshape(row_count, -1, head_dim)
    normed = grouped * lax.rsqrt(lax.optimization_barrier(jnp.mean(grouped * grouped, axis=2, keepdims=True)) + NORM_EPSILON)
    return (normed * gain.reshape(-1, head_dim)).reshape(row_count, -1)

def settle(values):
    return lax.optimization_barrier(values.astype(jnp.bfloat16)).astype(jnp.float32)

def reference(tokens, mix_gain, query_weight, key_weight, value_weight, outer_gate_weight, inner_gate_weight, conv_input_weight, query_gain, key_gain, gate_totals, conv_taps, attn_out_gain, conv_out_gain, attn_out_weight, conv_out_weight):
    widened = tokens.astype(jnp.float32)
    row_scale = lax.rsqrt(lax.optimization_barrier(jnp.sum(widened * widened, axis=1, keepdims=True)) / D + NORM_EPSILON)
    scaled = (widened * mix_gain).astype(jnp.bfloat16)

    def project(weight):
        return row_scale * jnp.dot(scaled, weight, preferred_element_type=jnp.float32)
    queries = settle(head_norm(project(query_weight), HEAD_DIM, query_gain))
    key_rows = settle(head_norm(project(key_weight), HEAD_DIM, key_gain))
    value_rows = settle(project(value_weight))
    query_span = math.gcd(SEQUENCE_TOKENS, 512)
    score_scale = HEAD_DIM ** (-0.5)
    positions = jnp.arange(SEQUENCE_TOKENS, dtype=jnp.int32)

    def one_head(head_index):
        offset = (head_index * HEAD_DIM).astype(jnp.int32)
        head_queries = lax.dynamic_slice_in_dim(queries, offset, HEAD_DIM, 1)
        head_keys = lax.dynamic_slice_in_dim(key_rows, offset, HEAD_DIM, 1)
        head_values = lax.dynamic_slice_in_dim(value_rows, offset, HEAD_DIM, 1)
        head_gates = lax.dynamic_slice_in_dim(gate_totals, head_index.astype(jnp.int32), 1, 1)[:, 0]

        def one_block(block_index):
            start = (block_index * query_span).astype(jnp.int32)
            block_queries = lax.dynamic_slice_in_dim(head_queries, start, query_span, 0)
            block_gates = lax.dynamic_slice_in_dim(head_gates, start, query_span, 0)
            scores = jnp.dot(block_queries, head_keys.T, precision=lax.Precision.HIGHEST) * score_scale
            scores = scores + block_gates[:, None] - head_gates[None, :]
            allowed = positions[None, :] <= (start + jnp.arange(query_span, dtype=jnp.int32))[:, None]
            row_max = lax.optimization_barrier(jnp.max(jnp.where(allowed, scores, -jnp.inf), axis=1, keepdims=True))
            weights = settle(jnp.where(allowed, jnp.exp(scores - row_max), 0.0))
            return jnp.dot(weights, head_values, precision=lax.Precision.HIGHEST)
        blocks = lax.map(one_block, jnp.arange(SEQUENCE_TOKENS // query_span, dtype=jnp.int32))
        return blocks.reshape(SEQUENCE_TOKENS, HEAD_DIM)
    attended = lax.map(one_head, jnp.arange(ATTENTION_HEADS, dtype=jnp.int32))
    attended = jnp.transpose(attended, (1, 0, 2)).reshape(SEQUENCE_TOKENS, ATTN_WIDTH)
    attn_mixed = head_norm(attended, HEAD_DIM, attn_out_gain).astype(jnp.bfloat16)
    gated = settle(project(inner_gate_weight) * project(conv_input_weight))
    padded = jnp.concatenate([jnp.zeros((CONV_K - 1, CONV_WIDTH), jnp.float32), gated], axis=0)
    convolved = conv_taps[0] * padded[0:SEQUENCE_TOKENS]
    for tap_index in range(1, CONV_K):
        convolved = convolved + conv_taps[tap_index] * padded[tap_index:tap_index + SEQUENCE_TOKENS]
    conv_mixed = head_norm(project(outer_gate_weight) * convolved, HEAD_DIM, conv_out_gain).astype(jnp.bfloat16)
    attn_slice = ATTN_WIDTH // N_TP
    conv_slice = CONV_WIDTH // N_TP
    total = jnp.zeros((SEQUENCE_TOKENS, D), jnp.float32)
    for slice_index in range(N_TP):
        attn_lo = slice_index * attn_slice
        conv_lo = slice_index * conv_slice
        partial_value = jnp.dot(attn_mixed[:, attn_lo:attn_lo + attn_slice], attn_out_weight[attn_lo:attn_lo + attn_slice], preferred_element_type=jnp.float32)
        partial_value = partial_value + jnp.dot(conv_mixed[:, conv_lo:conv_lo + conv_slice], conv_out_weight[conv_lo:conv_lo + conv_slice], preferred_element_type=jnp.float32)
        total = total + settle(partial_value)
    return total.astype(jnp.bfloat16)
```

```python
import jax
import jax.numpy as jnp
from jax import lax
from jax.experimental import pallas as pl
from jax.experimental.pallas import tpu as pltpu
from jax.sharding import PartitionSpec as P

NORM_EPSILON = 1e-06
LOG2_E = 1.4426950408889634
ROW_CHUNKS = 2
QUERY_TILE = 512
F32 = jnp.float32
BF16 = jnp.bfloat16


def swapped(shard, axis, offset):
    devices = lax.axis_size(axis)
    return lax.ppermute(shard, axis, [(i, i ^ offset) for i in range(devices)])


def xor_offsets(count):
    offsets = [0]
    bit = count >> 1
    while bit:
        offsets = offsets + [o ^ bit for o in offsets]
        bit >>= 1
    return offsets


def spread(shard, axis):
    pieces = [shard]
    bit = lax.axis_size(axis) >> 1
    while bit:
        pieces = pieces + [swapped(piece, axis, bit) for piece in pieces]
        bit >>= 1
    return pieces


def vmem_call(body, out_shape, operands, scalars=0, scratch=(), flops=0, limit=16):
    specs = [pl.BlockSpec(memory_space=pltpu.SMEM)] * scalars
    specs += [pl.BlockSpec(memory_space=pltpu.VMEM)] * (len(operands) - scalars)
    many = isinstance(out_shape, (list, tuple))
    out_specs = [pl.BlockSpec(memory_space=pltpu.VMEM)] * len(out_shape) if many else pl.BlockSpec(memory_space=pltpu.VMEM)
    return pl.pallas_call(
        body,
        out_shape=out_shape,
        in_specs=specs,
        out_specs=out_specs,
        scratch_shapes=list(scratch),
        compiler_params=pltpu.CompilerParams(vmem_limit_bytes=limit * 1024 * 1024),
        cost_estimate=pl.CostEstimate(flops=flops, transcendentals=0, bytes_accessed=1 << 20),
    )(*operands)


def dot_tn(left, right):
    return lax.dot_general(left, right, (((0,), (0,)), ((), ())), preferred_element_type=F32)


def dot_nn(left, right):
    return lax.dot_general(left, right, (((1,), (0,)), ((), ())), preferred_element_type=F32)


def column_norm(values):
    return values * lax.rsqrt(jnp.mean(values * values, axis=0, keepdims=True) + NORM_EPSILON)


def exchanged(shard, axis, groups):
    return lax.all_to_all(shard, axis, 0, 0, axis_index_groups=groups)


def project(ids, pieces, squares, weights, finish, out_shape, extra):
    rows, features = pieces[0].shape
    width = weights[0].shape[0]
    count = len(pieces)

    def body(ids_ref, *refs):
        piece_refs = refs[:count]
        squares_ref = refs[count]
        weight_refs = refs[count + 1 : count + 4]
        extra_refs = refs[count + 4 : count + 4 + len(extra)]
        outs, held = refs[count + 4 + len(extra) : -1], refs[-1]
        for offset, piece_ref in zip(xor_offsets(count), piece_refs):
            start = pl.multiple_of((ids_ref[1] ^ offset) * features, features)
            held[:, pl.ds(start, features)] = piece_ref[...]
        row_scale = lax.rsqrt(squares_ref[...] / width + NORM_EPSILON)
        kept = None
        for index, weight_ref in enumerate(weight_refs):
            product = dot_nn(held[...], weight_ref[...]).T * row_scale
            kept = finish(index, product, extra_refs, outs, kept)

    return vmem_call(
        body,
        out_shape,
        [ids, *pieces, squares, *weights, *extra],
        scalars=1,
        scratch=[pltpu.VMEM((rows, width), BF16)],
        flops=2 * sum(w.shape[1] for w in weights) * rows * width,
        limit=20,
    )


def project_heads(ids, pieces, squares, weights, gains, earlier, head_dim):
    rows = pieces[0].shape[0]
    head_count = weights[0].shape[1] // head_dim
    before = 0 if earlier is None else earlier.shape[2]

    def finish(index, product, extra_refs, outs, kept):
        query_out, pair_out = outs
        if index == 0 and before:
            query_out[:, :, :before] = extra_refs[2][...]
        for head in range(head_count):
            part = product[head * head_dim : (head + 1) * head_dim]
            if index == 0:
                query_out[head, :, before:] = (column_norm(part) * extra_refs[0][...]).astype(BF16)
            elif index == 1:
                pair_out[head, 0:head_dim, :] = (column_norm(part) * extra_refs[1][...]).astype(BF16)
            else:
                pair_out[head, head_dim : 2 * head_dim, :] = part.astype(BF16)

    out_shape = [
        jax.ShapeDtypeStruct((head_count, head_dim, before + rows), BF16),
        jax.ShapeDtypeStruct((head_count, 2 * head_dim, rows), BF16),
    ]
    extra = [*gains] + ([earlier] if before else [])
    return project(ids, pieces, squares, weights, finish, out_shape, extra)


def project_conv(ids, pieces, squares, weights):
    rows = pieces[0].shape[0]
    channels = weights[0].shape[1]

    def finish(index, product, extra_refs, outs, kept):
        if index == 0:
            outs[0][...] = product
        elif index == 1:
            return product
        else:
            outs[1][...] = (kept * product).astype(BF16)

    out_shape = [jax.ShapeDtypeStruct((channels, rows), F32), jax.ShapeDtypeStruct((channels, rows), BF16)]
    return project(ids, pieces, squares, weights, finish, out_shape, [])


def finish_conv(outers, gateds, prior, taps, gain, group, tile_count):
    channels, chunk_rows = gateds[0].shape
    count = len(gateds)
    rows = chunk_rows * count
    tail = prior.shape[1]
    tap_count = taps.shape[1]
    tile_rows = rows // tile_count

    def body(*refs):
        outer_refs, gated_refs = refs[:count], refs[count : 2 * count]
        prior_ref, taps_ref, gain_ref, out = refs[2 * count :]
        lane = lax.broadcasted_iota(jnp.int32, (group, tail), 1)
        for index in range(channels // group):
            span = slice(index * group, (index + 1) * group)
            values = jnp.concatenate([ref[span, :].astype(F32) for ref in gated_refs], axis=1)
            outer = jnp.concatenate([ref[span, :] for ref in outer_refs], axis=1)
            before = prior_ref[span, :].astype(F32)
            weights = taps_ref[span, :]
            total = weights[:, tap_count - 1 : tap_count] * values
            for back in range(1, tap_count):
                moved = pltpu.roll(values, back, 1)
                head = jnp.where(lane < back, pltpu.roll(before, back, 1), moved[:, :tail])
                moved = jnp.concatenate([head, moved[:, tail:]], axis=1)
                total = total + weights[:, tap_count - 1 - back : tap_count - back] * moved
            mixed = (column_norm(outer * total) * gain_ref[span, :]).astype(BF16)
            for tile in range(tile_count):
                out[tile, span, :] = mixed[:, tile * tile_rows : (tile + 1) * tile_rows]

    return vmem_call(
        body,
        jax.ShapeDtypeStruct((tile_count, channels, tile_rows), BF16),
        [*outers, *gateds, prior, taps, gain],
        flops=1 << 20,
    )


def attend(ids, queries, pairs, gates, gain, lane_count, tile_count):
    chunk_count = len(pairs[0])
    slot_count, head_dim, rows = queries.shape
    chunk_rows = rows // chunk_count
    tile_rows = rows // tile_count
    q_tile = min(QUERY_TILE, chunk_rows)
    k_tile = q_tile
    q_tiles = rows // q_tile
    per_chunk = chunk_rows // k_tile
    block_count = slot_count * lane_count
    wide = 2 * head_dim
    inverse_scale = float(head_dim) ** 0.5
    exponent_scale = LOG2_E / inverse_scale
    subtiles = q_tile // tile_rows

    def body(ids_ref, *refs):
        query_ref = refs[0]
        pair_refs = [refs[1 + chunk_count * l : 1 + chunk_count * (l + 1)] for l in range(lane_count)]
        cursor = 1 + chunk_count * lane_count
        gate_refs = refs[cursor : cursor + lane_count]
        gain_ref, out, key_store, value_store, query_store, score_store = refs[cursor + lane_count :]
        own = ids_ref[0]
        own_slot = own // lane_count
        own_lane = own % lane_count
        query_lane = jnp.where(own_slot % 2 == 0, own_lane, lane_count - 1 - own_lane)

        row8 = lax.broadcasted_iota(jnp.int32, (8, k_tile), 0)
        filler = jnp.zeros((head_dim - 8, k_tile), F32)
        for lane in range(lane_count):
            for slot in range(slot_count):
                block = slot * lane_count + (own_lane ^ lane)
                for chunk in range(chunk_count):
                    for part in range(per_chunk):
                        span = slice(part * k_tile, (part + 1) * k_tile)
                        at = chunk * chunk_rows + part * k_tile
                        index = block * q_tiles + chunk * per_chunk + part
                        ref = pair_refs[lane][chunk]
                        gate = gate_refs[lane][pl.ds(own_slot ^ slot, 1), at : at + k_tile] * (-inverse_scale)
                        first = gate.astype(BF16).astype(F32)
                        rest = gate - first
                        second = rest.astype(BF16).astype(F32)
                        third = rest - second
                        gate_rows = jnp.where(row8 == 0, first, jnp.where(row8 == 1, second, jnp.where(row8 == 2, third, 0.0)))
                        stacked = jnp.concatenate([ref[slot, 0:head_dim, span].astype(F32), gate_rows, filler], axis=0)
                        key_store[index] = stacked.T.astype(BF16)
                        value_store[index] = ref[slot, head_dim : 2 * head_dim, span]
        ones = (lax.broadcasted_iota(jnp.int32, (head_dim, q_tile), 0) < 3).astype(F32).astype(BF16)
        for slot in range(slot_count):
            for part in range(q_tiles):
                index = slot * q_tiles + part
                query_store[index, 0:head_dim, :] = query_ref[slot, :, part * q_tile : (part + 1) * q_tile]
                query_store[index, head_dim : 2 * head_dim, :] = ones

        key_at = lax.broadcasted_iota(jnp.int32, (k_tile, q_tile), 0)
        query_at = lax.broadcasted_iota(jnp.int32, (k_tile, q_tile), 1)
        head_gain = gain_ref[own_slot]

        def one_tile(step, _):
            slot = step // q_tiles
            block = slot * lane_count + jnp.where(slot % 2 == 0, query_lane, lane_count - 1 - query_lane)
            index = block * q_tiles + step % q_tiles
            query = query_store[step]

            def score(tile, place, top, masked=False):
                scores = dot_nn(key_store[tile], query)
                if masked:
                    scores = jnp.where(key_at <= query_at, scores, -1e30)
                score_store[place] = scores
                return jnp.maximum(top, jnp.max(scores, axis=0, keepdims=True))

            def absorb(tile, place, old_top, top, total):
                weights = jnp.exp2((score_store[place] - top) * exponent_scale).astype(BF16)
                factor = jnp.exp2((old_top - top) * exponent_scale)
                return total * factor + dot_nn(value_store[tile], weights)

            first = jnp.full((1, q_tile), -1e30, F32)
            total = jnp.zeros((head_dim, q_tile), F32)
            top = score(index, 0, first, True)

            def two_tiles(pair, carry):
                older, old, total = carry
                tile = 2 * pair
                before = jnp.where(pair == 0, index, tile - 1)
                middle = score(tile, 1, old)
                total = absorb(before, 0, older, old, total)
                latest = score(tile + 1, 0, middle)
                total = absorb(tile, 1, old, middle, total)
                return middle, latest, total

            older, old, total = lax.fori_loop(0, index // 2, two_tiles, (first, top, total))
            before = jnp.where(index < 2, index, index // 2 * 2 - 1)

            def odd_end():
                latest = score(index - 1, 1, old)
                return absorb(index - 1, 1, old, latest, absorb(before, 0, older, old, total))

            total = lax.cond(index % 2 == 1, odd_end, lambda: absorb(before, 0, older, old, total))
            mixed = (column_norm(total) * head_gain).astype(BF16)
            for sub in range(subtiles):
                out[step * subtiles + sub] = mixed[:, sub * tile_rows : (sub + 1) * tile_rows]
            return 0

        lax.fori_loop(0, slot_count * q_tiles, one_tile, 0)

    return vmem_call(
        body,
        jax.ShapeDtypeStruct((slot_count * tile_count, head_dim, tile_rows), BF16),
        [ids, queries, *[kv for lane in pairs for kv in lane], *gates, gain],
        scalars=1,
        scratch=[
            pltpu.VMEM((block_count * q_tiles, k_tile, wide), BF16),
            pltpu.VMEM((block_count * q_tiles, head_dim, k_tile), BF16),
            pltpu.VMEM((slot_count * q_tiles, wide, q_tile), BF16),
            pltpu.VMEM((2, k_tile, q_tile), F32),
        ],
        flops=4 * head_dim * slot_count * rows * block_count * rows,
        limit=20,
    )


def output_rows(ids, pieces, weights, base, out_dtype):
    source_count = len(weights)
    piece_count, piece_height, rows = pieces.shape
    slot_count = piece_count // source_count
    height = slot_count * piece_height
    width = weights[0].shape[1]
    offsets = xor_offsets(source_count)
    has_base = base is not None

    def body(ids_ref, piece_ref, *refs):
        weight_refs = refs[:source_count]
        held, out_ref = refs[-1], refs[-2]
        for place, offset in enumerate(offsets):
            source = ids_ref[1] ^ offset
            for slot in range(slot_count):
                start = place * height + slot * piece_height
                held[start : start + piece_height, :] = piece_ref[slot * source_count + source]
        total = refs[source_count][...] if has_base else None
        for place in range(source_count):
            part = dot_tn(held[place * height : (place + 1) * height, :], weight_refs[place][...])
            total = part if total is None else total + part
        out_ref[...] = total.astype(out_dtype)

    return vmem_call(
        body,
        jax.ShapeDtypeStruct((rows, width), out_dtype),
        [ids, pieces, *weights] + ([base] if has_base else []),
        scalars=1,
        scratch=[pltpu.VMEM((source_count * height, rows), BF16)],
        flops=2 * source_count * height * rows * width,
    )


def per_device(
    tokens,
    mix_gain,
    query_weight,
    key_weight,
    value_weight,
    outer_gate_weight,
    inner_gate_weight,
    conv_input_weight,
    query_gain,
    key_gain,
    gate_totals,
    conv_taps,
    attn_out_gain,
    conv_out_gain,
    attn_out_weight,
    conv_out_weight,
):
    rows, features = tokens.shape
    head_dim = query_gain.shape[0]
    head_count = query_weight.shape[1] // head_dim
    sp_count = lax.axis_size("sp")
    tp_count = lax.axis_size("tp")
    lane_count = sp_count // head_count
    sp_index = lax.axis_index("sp")
    tp_index = lax.axis_index("tp")
    ids = jnp.stack([sp_index, tp_index]).astype(jnp.int32)
    chunk_rows = rows // ROW_CHUNKS
    straight = [[slot * lane_count + lane for slot in range(head_count)] for lane in range(lane_count)]
    snaked = [
        [slot * lane_count + (lane_count - 1 - lane if slot % 2 else lane) for slot in range(head_count)]
        for lane in range(lane_count)
    ]
    snaked_wide = [[p * tp_count + t for p in group for t in range(tp_count)] for group in snaked]

    own_gain = lax.dynamic_slice_in_dim(mix_gain, tp_index * features, features, 0)
    scaled = [
        (tokens[c * chunk_rows : (c + 1) * chunk_rows].astype(F32) * own_gain).astype(BF16) for c in range(ROW_CHUNKS)
    ]
    far = []
    for c in range(ROW_CHUNKS):
        far.append(swapped(scaled[c], "tp", tp_count >> 1))
    tokens, gate_totals = lax.optimization_barrier((tokens, gate_totals, *scaled))[:2]
    widened = tokens.astype(F32)
    squares = jnp.sum(widened * widened, axis=1).reshape(1, rows)
    bit = tp_count >> 1
    while bit:
        squares = squares + swapped(squares, "tp", bit)
        bit >>= 1
    gains = (query_gain.reshape(-1, 1), key_gain.reshape(-1, 1))
    far[0], squares, ids, gains = lax.optimization_barrier((far[0], squares, ids, gains))
    chunks = []
    for c in range(ROW_CHUNKS):
        pieces = [scaled[c], far[c]]
        bit = tp_count >> 2
        while bit:
            pieces = pieces + [swapped(piece, "tp", bit) for piece in pieces]
            bit >>= 1
        chunks.append(pieces)

    attn_weight = (query_weight, key_weight, value_weight)
    conv_weight = (outer_gate_weight, inner_gate_weight, conv_input_weight)
    queries, outers, gateds = None, [], []
    pairs = [[] for _ in range(lane_count)]
    for c in range(ROW_CHUNKS):
        chunk_squares = squares[:, c * chunk_rows : (c + 1) * chunk_rows]
        queries, chunk_pairs = project_heads(ids, chunks[c], chunk_squares, attn_weight, gains, queries, head_dim)
        moved = exchanged(chunk_pairs, "sp", straight)
        pairs[0].append(moved)
        for lane in range(1, lane_count):
            pairs[lane].append(swapped(moved, "sp", lane))
    for c in range(ROW_CHUNKS):
        chunk_squares = squares[:, c * chunk_rows : (c + 1) * chunk_rows]
        outer, gated = project_conv(ids, chunks[c], chunk_squares, conv_weight)
        outers.append(outer)
        gateds.append(gated)
    tail = min(128, chunk_rows)
    prior = lax.ppermute(gateds[-1][:, chunk_rows - tail :], "sp", [(i, i + 1) for i in range(sp_count - 1)])
    queries = exchanged(queries, "sp", snaked)

    own_gates = gate_totals.T
    own_slot = sp_index // lane_count
    slot_gates = []
    for offset in range(head_count):
        wanted = lax.dynamic_slice_in_dim(own_gates, own_slot ^ offset, 1, 0)
        slot_gates.append(swapped(wanted, "sp", offset * lane_count) if offset else wanted)
    slot_gates = jnp.concatenate(slot_gates, axis=0)
    gates = [slot_gates]
    for lane in range(1, lane_count):
        gates.append(swapped(slot_gates, "sp", lane))

    attn_out_weight, conv_out_weight = lax.optimization_barrier((attn_out_weight, conv_out_weight, far[-1]))[:2]
    attn_rows = spread(attn_out_weight, "tp")
    conv_rows = spread(conv_out_weight, "tp")

    conv_mixed = finish_conv(
        outers, gateds, prior, conv_taps.T, conv_out_gain.reshape(-1, 1), head_dim, tp_count
    )
    conv_pieces = lax.all_to_all(conv_mixed, "tp", 0, 0)
    base = output_rows(ids, conv_pieces, conv_rows, None, F32)

    attended = attend(ids, queries, pairs, gates, attn_out_gain.reshape(head_count, head_dim, 1), lane_count, tp_count)
    attn_pieces = lax.all_to_all(attended, ("sp", "tp"), 0, 0, axis_index_groups=snaked_wide)
    return output_rows(ids, attn_pieces, attn_rows, base, BF16)


def solution(mesh):
    placed = (
        P("sp", "tp"),
        P(),
        P(None, "tp"),
        P(None, "tp"),
        P(None, "tp"),
        P(None, "tp"),
        P(None, "tp"),
        P(None, "tp"),
        P(),
        P(),
        P("sp", "tp"),
        P(None, "tp"),
        P("tp"),
        P("tp"),
        P("tp", None),
        P("tp", None),
    )
    return jax.shard_map(per_device, mesh=mesh, in_specs=placed, out_specs=P(("sp", "tp"), None), check_vma=False)
```

```python
import jax
import jax.numpy as jnp
from jax import lax
from jax.experimental import pallas as pl
from jax.experimental.pallas import tpu as pltpu
from jax.sharding import PartitionSpec as P

NORM_EPSILON = 1e-06
LOG2_E = 1.4426950408889634
ROW_CHUNKS = 2
QUERY_TILE = 512
OUTPUT_PARTS = 4
F32 = jnp.float32
BF16 = jnp.bfloat16


def swapped(shard, axis, offset):
    devices = lax.axis_size(axis)
    return lax.ppermute(shard, axis, [(i, i ^ offset) for i in range(devices)])


def xor_offsets(count):
    offsets = [0]
    bit = count >> 1
    while bit:
        offsets = offsets + [o ^ bit for o in offsets]
        bit >>= 1
    return offsets


def in_hbm(x):
    return pltpu.with_memory_space_constraint(x, pltpu.HBM) if x.size >= 1 << 14 else x


def vmem_call(body, out_shape, operands, scalars=0, scratch=(), flops=0, limit=16, outside=(), resident=(), out_space=pltpu.VMEM):
    specs = [pl.BlockSpec(memory_space=pltpu.SMEM)] * scalars
    specs += [
        pl.BlockSpec(memory_space=pl.ANY if any(x is o for o in outside) else pltpu.VMEM) for x in operands[scalars:]
    ]
    many = isinstance(out_shape, (list, tuple))
    shapes = [pltpu.HBM(x.shape, x.dtype) for x in (out_shape if many else [out_shape])]
    out_specs = [pl.BlockSpec(memory_space=out_space)] * len(shapes)
    return pl.pallas_call(
        body,
        out_shape=shapes if many else shapes[0],
        in_specs=specs,
        out_specs=out_specs if many else out_specs[0],
        scratch_shapes=list(scratch),
        compiler_params=pltpu.CompilerParams(vmem_limit_bytes=limit * 1024 * 1024),
        cost_estimate=pl.CostEstimate(flops=flops, transcendentals=0, bytes_accessed=1 << 20),
    )(
        *[
            pltpu.with_memory_space_constraint(x, pltpu.VMEM) if any(x is r for r in resident) else in_hbm(x)
            for x in operands
        ]
    )


class Arrival:
    def __init__(self, sources, target, arrived):
        self.copies = [pltpu.make_async_copy(ref, target.at[i], arrived.at[i]) for i, ref in enumerate(sources)]
        for copy in self.copies:
            copy.start()

    def wait(self, index):
        self.copies[index].wait()


def dot_nn(left, right):
    return lax.dot_general(left, right, (((1,), (0,)), ((), ())), preferred_element_type=F32)


def column_norm(values):
    return values * lax.rsqrt(jnp.mean(values * values, axis=0, keepdims=True) + NORM_EPSILON)


def exchanged(shard, axis, groups):
    return lax.all_to_all(shard, axis, 0, 0, axis_index_groups=groups)


def staged(weights):
    def body(*refs):
        out, arrived = refs[-2:]
        arrival = Arrival(refs[:-2], out, arrived)
        for index in range(len(weights)):
            arrival.wait(index)

    return pl.pallas_call(
        body,
        out_shape=pltpu.VMEM((len(weights), *weights[0].shape), weights[0].dtype),
        in_specs=[pl.BlockSpec(memory_space=pl.ANY)] * len(weights),
        out_specs=pl.BlockSpec(memory_space=pltpu.VMEM),
        scratch_shapes=[pltpu.SemaphoreType.DMA((len(weights),))],
        compiler_params=pltpu.CompilerParams(vmem_limit_bytes=8 * 1024 * 1024),
        name="staged",
    )(*[in_hbm(w) for w in weights])


def project(ids, chunks, squares, weights, finish, out_shape, extra):
    rows, features = chunks[0][0].shape
    resident = not isinstance(weights, (list, tuple))
    weight_count = weights.shape[0] if resident else len(weights)
    width, channels = weights.shape[1:] if resident else weights[0].shape
    chunk_count, count = len(chunks), len(chunks[0])
    pieces = [piece for chunk in chunks for piece in chunk]
    weight_list = [weights] if resident else list(weights)

    def body(ids_ref, *refs):
        piece_refs, refs = refs[: len(pieces)], refs[len(pieces) :]
        squares_ref, refs = refs[0], refs[1:]
        weight_refs, refs = refs[: len(weight_list)], refs[len(weight_list) :]
        extra_refs, refs = refs[: len(extra)], refs[len(extra) :]
        outs, refs = refs[: len(out_shape)], refs[len(out_shape) :]
        held, product_store, joined = refs[:3]
        copies = []
        for chunk in range(chunk_count):
            for place, offset in enumerate(xor_offsets(count)):
                start = pl.multiple_of((ids_ref[1] ^ offset) * features, features)
                index = chunk * count + place
                copies.append(
                    pltpu.make_async_copy(
                        piece_refs[index], held.at[chunk, :, pl.ds(start, features)], joined.at[index]
                    )
                )
        for copy in copies[:count]:
            copy.start()
        if not resident:
            weight_store, arrived = refs[3:]
            arrival = Arrival(weight_refs, weight_store, arrived)
        for copy in copies[count:]:
            copy.start()
        for chunk in range(chunk_count):
            for copy in copies[chunk * count : (chunk + 1) * count]:
                copy.wait()
            span = slice(chunk * rows, (chunk + 1) * rows)
            row_scale = lax.rsqrt(squares_ref[:, span] / width + NORM_EPSILON)
            for index in range(weight_count):
                if not resident and chunk == 0:
                    arrival.wait(index)
                weight = weight_refs[0][index] if resident else weight_store[index]
                product_store[index] = dot_nn(held[chunk], weight).T * row_scale
                finish(ids_ref, chunk, index, product_store, extra_refs, outs)

    scratch = [
        pltpu.VMEM((chunk_count, rows, width), BF16),
        pltpu.VMEM((weight_count, channels, rows), F32),
        pltpu.SemaphoreType.DMA((len(pieces),)),
    ]
    if not resident:
        scratch += [pltpu.VMEM((weight_count, width, channels), BF16), pltpu.SemaphoreType.DMA((weight_count,))]
    return vmem_call(
        body,
        out_shape,
        [ids, *pieces, squares, *weight_list, *extra],
        scalars=1,
        scratch=scratch,
        flops=2 * weight_count * channels * rows * chunk_count * width,
        limit=24,
        outside=pieces if resident else (*weights, *pieces),
        resident=weight_list if resident else (),
    )


def project_heads(ids, pieces, squares, weights, gains, earlier, head_dim, slot_step, split):
    rows = pieces[0].shape[0]
    head_count = weights.shape[2] // head_dim
    before = 0 if earlier is None else earlier.shape[2]

    def finish(ids_ref, chunk, index, product, extra_refs, outs):
        query_out, pair_outs = outs[0], outs[1:]
        if index == 0 and before:
            query_out[:, :, :before] = extra_refs[2][...]
        own_slot = ids_ref[0] // slot_step
        for head in range(head_count):
            base = head * head_dim
            if split and index:
                base = pl.multiple_of((own_slot ^ head) * head_dim, head_dim)
            part = product[index, pl.ds(base, head_dim), :]
            if index == 0:
                query_out[head, :, before:] = (column_norm(part) * extra_refs[0][...]).astype(BF16)
                continue
            settled = (column_norm(part) * extra_refs[1][...] if index == 1 else part).astype(BF16)
            span = slice((index - 1) * head_dim, index * head_dim)
            if split:
                pair_outs[head][span, :] = settled
            else:
                pair_outs[0][head, span, :] = settled

    out_shape = [jax.ShapeDtypeStruct((head_count, head_dim, before + rows), BF16)]
    if split:
        out_shape += [jax.ShapeDtypeStruct((2 * head_dim, rows), BF16)] * head_count
    else:
        out_shape += [jax.ShapeDtypeStruct((head_count, 2 * head_dim, rows), BF16)]
    extra = [*gains] + ([earlier] if before else [])
    outs = project(ids, [pieces], squares, weights, finish, out_shape, extra)
    return outs[0], outs[1:]


def project_conv(ids, chunks, squares, weights):
    chunk_rows = chunks[0][0].shape[0]
    rows = chunk_rows * len(chunks)
    channels = weights[0].shape[1]
    tail = min(128, chunk_rows)

    def finish(ids_ref, chunk, index, product, extra_refs, outs):
        span = slice(chunk * chunk_rows, (chunk + 1) * chunk_rows)
        if index == 0:
            outs[0][:, span] = product[0]
        elif index == 2:
            gated = (product[1] * product[2]).astype(BF16)
            outs[1][:, span] = gated
            if chunk == len(chunks) - 1:
                outs[2][...] = gated[:, chunk_rows - tail :]

    out_shape = [
        jax.ShapeDtypeStruct((channels, rows), F32),
        jax.ShapeDtypeStruct((channels, rows), BF16),
        jax.ShapeDtypeStruct((channels, tail), BF16),
    ]
    return project(ids, chunks, squares, weights, finish, out_shape, [])


def finish_conv(outers, gateds, prior, taps, gain, group, tile_count):
    channels, chunk_rows = gateds[0].shape
    count = len(gateds)
    rows = chunk_rows * count
    tail = prior.shape[1]
    tap_count = taps.shape[1]
    tile_rows = rows // tile_count

    def body(*refs):
        outer_refs, gated_refs = refs[:count], refs[count : 2 * count]
        prior_ref, taps_ref, gain_ref, out = refs[2 * count :]
        lane = lax.broadcasted_iota(jnp.int32, (group, tail), 1)
        for index in range(channels // group):
            span = slice(index * group, (index + 1) * group)
            values = jnp.concatenate([ref[span, :].astype(F32) for ref in gated_refs], axis=1)
            outer = jnp.concatenate([ref[span, :] for ref in outer_refs], axis=1)
            before = prior_ref[span, :].astype(F32)
            weights = taps_ref[span, :]
            total = weights[:, tap_count - 1 : tap_count] * values
            for back in range(1, tap_count):
                moved = pltpu.roll(values, back, 1)
                head = jnp.where(lane < back, pltpu.roll(before, back, 1), moved[:, :tail])
                moved = jnp.concatenate([head, moved[:, tail:]], axis=1)
                total = total + weights[:, tap_count - 1 - back : tap_count - back] * moved
            mixed = (column_norm(outer * total) * gain_ref[span, :]).astype(BF16)
            for tile in range(tile_count):
                out[tile, span, :] = mixed[:, tile * tile_rows : (tile + 1) * tile_rows]

    return vmem_call(
        body,
        jax.ShapeDtypeStruct((tile_count, channels, tile_rows), BF16),
        [*outers, *gateds, prior, taps, gain],
        flops=1 << 20,
    )


def attend(ids, queries, pairs, gates, gain, lane_count, tile_count):
    chunk_count = len(pairs[0])
    slot_count, head_dim, rows = queries.shape
    counts = [len(chunk) for chunk in pairs[0]]
    flat_pairs = [kv for lane in pairs for chunk in lane for kv in chunk]
    chunk_rows = rows // chunk_count
    tile_rows = rows // tile_count
    q_tile = min(QUERY_TILE, chunk_rows)
    k_tile = q_tile
    q_tiles = rows // q_tile
    per_chunk = chunk_rows // k_tile
    block_count = slot_count * lane_count
    steps = slot_count * q_tiles
    wide = 2 * head_dim
    exponent_scale = LOG2_E * float(head_dim) ** -0.5
    subtiles = q_tile // tile_rows
    blocks = [slot * lane_count + (lane_count - 1 if slot % 2 else 0) for slot in range(slot_count)]
    full_tiles = sum(block * q_tiles + part for block in blocks for part in range(q_tiles))
    unroll = next(n for n in (4, 2, 1) if full_tiles % n == 0)

    def body(ids_ref, *refs):
        query_ref, refs = refs[0], refs[1:]
        flat_refs, refs = refs[: len(flat_pairs)], refs[len(flat_pairs) :]
        gate_refs, refs = refs[:lane_count], refs[lane_count:]
        gain_ref, out, key_store, value_store, query_store, score_store = refs[:6]
        top_store, total_store, arrived = refs[6:9]
        stages = refs[9:]
        copies = [pltpu.make_async_copy(ref, stage, arrived.at[i]) for i, (ref, stage) in enumerate(zip(flat_refs, stages))]
        for copy in copies:
            copy.start()
        own = ids_ref[0]
        own_slot = own // lane_count
        own_lane = own % lane_count
        query_lane = jnp.where(own_slot % 2 == 0, own_lane, lane_count - 1 - own_lane)

        ones = (lax.broadcasted_iota(jnp.int32, (head_dim, q_tile), 0) < 3).astype(F32).astype(BF16)
        for slot in range(slot_count):
            for part in range(q_tiles):
                index = slot * q_tiles + part
                query = query_ref[slot, :, part * q_tile : (part + 1) * q_tile].astype(F32) * exponent_scale
                coarse = query.astype(BF16)
                query_store[index, 0:head_dim, :] = coarse
                query_store[index, head_dim:wide, :] = ones
                query_store[index, wide : wide + head_dim, :] = (query - coarse.astype(F32)).astype(BF16)
                query_store[index, wide + head_dim : 2 * wide, :] = jnp.zeros_like(coarse)

        row8 = lax.broadcasted_iota(jnp.int32, (8, k_tile), 0)
        filler = jnp.zeros((head_dim - 8, k_tile), F32)

        def settle(ref, slot, lane, chunk):
            block = slot * lane_count + (own_lane ^ lane)
            for part in range(per_chunk):
                span = slice(part * k_tile, (part + 1) * k_tile)
                at = chunk * chunk_rows + part * k_tile
                index = block * q_tiles + chunk * per_chunk + part
                gate = gate_refs[lane][pl.ds(slot, 1), at : at + k_tile] * (-LOG2_E)
                first = gate.astype(BF16).astype(F32)
                rest = gate - first
                second = rest.astype(BF16).astype(F32)
                third = rest - second
                gate_rows = jnp.where(row8 == 0, first, jnp.where(row8 == 1, second, jnp.where(row8 == 2, third, 0.0)))
                stacked = jnp.concatenate([ref[0:head_dim, span].astype(F32), gate_rows, filler], axis=0)
                key_store[index] = stacked.T.astype(BF16)
                value_store[index] = ref[head_dim:wide, span]

        cursor = 0
        for lane in range(lane_count):
            for chunk in range(chunk_count):
                for member in range(counts[chunk]):
                    copies[cursor].wait()
                    if counts[chunk] > 1:
                        settle(stages[cursor], own_slot ^ member, lane, chunk)
                    else:
                        for slot in range(slot_count):
                            settle(stages[cursor].at[slot], slot, lane, chunk)
                    cursor += 1

        def tile_of(step):
            slot = step // q_tiles
            block = slot * lane_count + jnp.where(slot % 2 == 0, query_lane, lane_count - 1 - query_lane)
            return block * q_tiles + step % q_tiles

        def score(step, tile, place, masked):
            keys = key_store[tile]
            scores = dot_nn(jnp.concatenate([keys, keys], axis=1), query_store[step])
            if masked:
                key_at = lax.broadcasted_iota(jnp.int32, (k_tile, q_tile), 0)
                query_at = lax.broadcasted_iota(jnp.int32, (k_tile, q_tile), 1)
                scores = jnp.where(key_at <= query_at, scores, -1e30)
            score_store[place] = scores
            highest = jnp.max(scores, axis=0, keepdims=True)
            if masked:
                top_store[step] = highest
                return highest, None
            old = top_store[step]
            top = jnp.maximum(old, highest)
            top_store[step] = top
            return top, jnp.exp2(old - top)

        def absorb(step, tile, place, top, factor):
            weights = jnp.exp2(score_store[place] - top).astype(BF16)
            added = dot_nn(value_store[tile], weights)
            total_store[step] = added if factor is None else total_store[step] * factor + added

        top, _ = score(0, tile_of(0), 0, True)

        def on_diagonal(pair, top):
            step = 2 * pair
            middle, _ = score(step + 1, tile_of(step + 1), 1, True)
            absorb(step, tile_of(step), 0, top, None)
            following = jnp.minimum(step + 2, steps - 1)
            latest, _ = score(following, tile_of(following), 0, True)
            absorb(step + 1, tile_of(step + 1), 1, middle, None)
            return latest

        lax.fori_loop(0, steps // 2, on_diagonal, top)

        def following(step, tile):
            done = tile + 1 >= tile_of(step)
            return jnp.where(done, jnp.minimum(step + 1, steps - 1), step), jnp.where(done, 0, tile + 1)

        step = jnp.where(tile_of(0) == 0, 1, 0)
        top, factor = score(step, 0, 0, False)

        def below(turn, carry):
            step, tile, top, factor = carry
            for count in range(unroll):
                next_step, next_tile = following(step, tile)
                place = count % 2
                if unroll == 1:
                    absorb(step, tile, 0, top, factor)
                    next_top, next_factor = score(next_step, next_tile, 0, False)
                elif count < unroll - 1:
                    next_top, next_factor = score(next_step, next_tile, 1 - place, False)
                    absorb(step, tile, place, top, factor)
                else:
                    more = turn + 1 < full_tiles // unroll
                    next_step = jnp.where(more, next_step, step)
                    next_tile = jnp.where(more, next_tile, tile)
                    next_top, next_factor = score(next_step, next_tile, 0, False)
                    absorb(step, tile, 1, top, factor)
                step, tile, top, factor = next_step, next_tile, next_top, next_factor
            return step, tile, top, factor

        lax.fori_loop(0, full_tiles // unroll, below, (step, jnp.int32(0), top, factor))

        head_gain = gain_ref[own_slot]
        for step in range(steps):
            mixed = (column_norm(total_store[step]) * head_gain).astype(BF16)
            for sub in range(subtiles):
                out[step * subtiles + sub] = mixed[:, sub * tile_rows : (sub + 1) * tile_rows]

    return vmem_call(
        body,
        jax.ShapeDtypeStruct((slot_count * tile_count, head_dim, tile_rows), BF16),
        [ids, queries, *flat_pairs, *gates, gain],
        scalars=1,
        scratch=[
            pltpu.VMEM((block_count * q_tiles, k_tile, wide), BF16),
            pltpu.VMEM((block_count * q_tiles, head_dim, k_tile), BF16),
            pltpu.VMEM((steps, 2 * wide, q_tile), BF16),
            pltpu.VMEM((2, k_tile, q_tile), F32),
            pltpu.VMEM((steps, 1, q_tile), F32),
            pltpu.VMEM((steps, head_dim, q_tile), F32),
            pltpu.SemaphoreType.DMA((len(flat_pairs),)),
            *[pltpu.VMEM(kv.shape, BF16) for kv in flat_pairs],
        ],
        flops=4 * head_dim * slot_count * rows * block_count * rows,
        limit=28,
        outside=flat_pairs,
    )


def output_rows(ids, pieces, weights, base):
    source_count = len(weights)
    piece_count, piece_height, rows = pieces.shape
    slot_count = piece_count // source_count
    height = slot_count * piece_height
    width = weights[0].shape[1]
    offsets = xor_offsets(source_count)
    bases = [] if base is None else [base]
    parts = OUTPUT_PARTS
    part_width = width // parts

    def body(ids_ref, piece_ref, *refs):
        weight_refs, refs = refs[:source_count], refs[source_count:]
        base_refs, refs = refs[: len(bases)], refs[len(bases) :]
        out_ref, held, weight_store, result, joined, arrived, left = refs[:7]
        gathers = []
        for place, offset in enumerate(offsets):
            source = ids_ref[1] ^ offset
            for slot in range(slot_count):
                start = place * height + slot * piece_height
                gathers.append(
                    pltpu.make_async_copy(
                        piece_ref.at[slot * source_count + source],
                        held.at[start : start + piece_height, :],
                        joined.at[place * slot_count + slot],
                    )
                )
                gathers[-1].start()
        arrival = Arrival(weight_refs, weight_store, arrived)
        if bases:
            below = pltpu.make_async_copy(base_refs[0], refs[7], refs[8].at[0])
            below.start()
        for copy in gathers:
            copy.wait()
        turned = held[...].T
        for place in range(source_count):
            arrival.wait(place)
        if bases:
            below.wait()
        stores = []
        for part in range(parts):
            span = slice(part * part_width, (part + 1) * part_width)
            weight = jnp.concatenate([weight_store[place, :, span] for place in range(source_count)], axis=0)
            total = dot_nn(turned, weight)
            if bases:
                total = total + refs[7][:, span].astype(F32)
            result[:, span] = total.astype(BF16)
            stores.append(pltpu.make_async_copy(result.at[:, span], out_ref.at[:, span], left.at[part]))
            stores[-1].start()
        for copy in stores:
            copy.wait()

    scratch = [
        pltpu.VMEM((source_count * height, rows), BF16),
        pltpu.VMEM((source_count, height, width), BF16),
        pltpu.VMEM((rows, width), BF16),
        pltpu.SemaphoreType.DMA((piece_count,)),
        pltpu.SemaphoreType.DMA((source_count,)),
        pltpu.SemaphoreType.DMA((parts,)),
    ]
    if bases:
        scratch += [pltpu.VMEM((rows, width), BF16), pltpu.SemaphoreType.DMA((1,))]
    return vmem_call(
        body,
        jax.ShapeDtypeStruct((rows, width), BF16),
        [ids, pieces, *weights, *bases],
        scalars=1,
        scratch=scratch,
        flops=2 * source_count * height * rows * width,
        outside=(pieces, *weights, *bases),
        out_space=pl.ANY,
    )


def per_device(
    tokens,
    mix_gain,
    query_weight,
    key_weight,
    value_weight,
    outer_gate_weight,
    inner_gate_weight,
    conv_input_weight,
    query_gain,
    key_gain,
    gate_totals,
    conv_taps,
    attn_out_gain,
    conv_out_gain,
    attn_out_weight,
    conv_out_weight,
):
    rows, features = tokens.shape
    head_dim = query_gain.shape[0]
    head_count = query_weight.shape[1] // head_dim
    sp_count = lax.axis_size("sp")
    tp_count = lax.axis_size("tp")
    lane_count = sp_count // head_count
    sp_index = lax.axis_index("sp")
    tp_index = lax.axis_index("tp")
    ids = jnp.stack([sp_index, tp_index]).astype(jnp.int32)
    chunk_rows = rows // ROW_CHUNKS
    straight = [[slot * lane_count + lane for slot in range(head_count)] for lane in range(lane_count)]
    snaked = [
        [slot * lane_count + (lane_count - 1 - lane if slot % 2 else lane) for slot in range(head_count)]
        for lane in range(lane_count)
    ]
    snaked_wide = [[p * tp_count + t for p in group for t in range(tp_count)] for group in snaked]

    own_gain = lax.dynamic_slice_in_dim(mix_gain, tp_index * features, features, 0)
    scaled = [
        (tokens[c * chunk_rows : (c + 1) * chunk_rows].astype(F32) * own_gain).astype(BF16) for c in range(ROW_CHUNKS)
    ]
    far = []
    for c in range(ROW_CHUNKS):
        far.append(swapped(scaled[c], "tp", tp_count >> 1))
    tokens, gate_totals = lax.optimization_barrier((tokens, gate_totals, *scaled))[:2]
    widened = tokens.astype(F32)
    squares = jnp.sum(widened * widened, axis=1).reshape(1, rows)
    gains = (query_gain.reshape(-1, 1), key_gain.reshape(-1, 1))
    out_gains = (attn_out_gain.reshape(head_count, head_dim, 1), conv_out_gain.reshape(-1, 1), conv_taps.T)
    slot_gates = exchanged(gate_totals.T, "sp", straight)
    gates = [slot_gates] + [swapped(slot_gates, "sp", lane) for lane in range(1, lane_count)]
    attn_weight = staged((query_weight, key_weight, value_weight))
    conv_weight = (outer_gate_weight, inner_gate_weight, conv_input_weight)
    squares, ids, gains, out_gains, gates, attn_weight = lax.optimization_barrier(
        (squares, ids, gains, out_gains, gates, attn_weight)
    )
    bit = tp_count >> 1
    while bit:
        squares = squares + swapped(squares, "tp", bit)
        bit >>= 1
    chunks = []
    for c in range(ROW_CHUNKS):
        pieces = [scaled[c], far[c]]
        bit = tp_count >> 2
        while bit:
            pieces = pieces + [swapped(piece, "tp", bit) for piece in pieces]
            bit >>= 1
        chunks.append(pieces)

    queries, outers, gateds = None, [], []
    pairs = [[] for _ in range(lane_count)]
    for c in range(ROW_CHUNKS):
        chunk_squares = squares[:, c * chunk_rows : (c + 1) * chunk_rows]
        split = c > 0
        if split:
            chunk_squares, outers[-1] = lax.optimization_barrier((chunk_squares, outers[-1]))
        queries, own_pairs = project_heads(
            ids, chunks[c], chunk_squares, attn_weight, gains, queries, head_dim, lane_count, split
        )
        outer, gated, gated_tail = project_conv(ids, [chunks[c]], chunk_squares, conv_weight)
        outers.append(outer)
        gateds.append(gated)
        if split:
            moved = [swapped(p, "sp", i * lane_count) if i else p for i, p in enumerate(own_pairs)]
        else:
            moved = [exchanged(own_pairs[0], "sp", straight)]
        pairs[0].append(moved)
        for lane in range(1, lane_count):
            through = []
            for p in moved:
                through.append(swapped(p, "sp", lane))
            pairs[lane].append(through)
    prior = lax.ppermute(gated_tail, "sp", [(i, i + 1) for i in range(sp_count - 1)])
    queries = exchanged(queries, "sp", snaked)

    far_weights = lax.optimization_barrier((attn_out_weight, conv_out_weight, far[-1]))[:2]
    half = tp_count >> 1
    far_weights = [swapped(weight, "tp", half) for weight in far_weights]

    conv_mixed = finish_conv(
        outers, gateds, prior, out_gains[2], out_gains[1], head_dim, tp_count
    )
    conv_pieces = lax.all_to_all(conv_mixed, "tp", 0, 0)
    attended = attend(
        ids, queries, pairs, gates, out_gains[0], lane_count, tp_count
    )
    attn_pieces = lax.all_to_all(attended, ("sp", "tp"), 0, 0, axis_index_groups=snaked_wide)
    own_weights = lax.optimization_barrier((attn_out_weight, conv_out_weight, *far_weights, attended))[:4]
    gathered = []
    for own, distant in zip(own_weights[:2], own_weights[2:]):
        parts = [own, distant]
        bit = tp_count >> 2
        while bit:
            parts = parts + [swapped(part, "tp", bit) for part in parts]
            bit >>= 1
        gathered.append(parts)
    base = output_rows(ids, conv_pieces, gathered[1], None)
    return output_rows(ids, attn_pieces, gathered[0], base)


def solution(mesh):
    placed = (
        P("sp", "tp"),
        P(),
        P(None, "tp"),
        P(None, "tp"),
        P(None, "tp"),
        P(None, "tp"),
        P(None, "tp"),
        P(None, "tp"),
        P(),
        P(),
        P("sp", "tp"),
        P(None, "tp"),
        P("tp"),
        P("tp"),
        P("tp", None),
        P("tp", None),
    )
    return jax.shard_map(per_device, mesh=mesh, in_specs=placed, out_specs=P(("sp", "tp"), None), check_vma=False)
```

```python
import jax
import jax.numpy as jnp
from jax import lax
from jax.experimental import pallas as pl
from jax.experimental.pallas import tpu as pltpu
from jax.sharding import PartitionSpec as P

NORM_EPSILON = 1e-06
LOG2_E = 1.4426950408889634
ROW_CHUNKS = 2
QUERY_TILE = 512
OUTPUT_PARTS = 4
F32 = jnp.float32
BF16 = jnp.bfloat16


def swapped(shard, axis, offset):
    devices = lax.axis_size(axis)
    return lax.ppermute(shard, axis, [(i, i ^ offset) for i in range(devices)])


def xor_offsets(count):
    offsets = [0]
    bit = count >> 1
    while bit:
        offsets = offsets + [o ^ bit for o in offsets]
        bit >>= 1
    return offsets


def in_hbm(x):
    return pltpu.with_memory_space_constraint(x, pltpu.HBM) if x.size >= 1 << 14 else x


def vmem_call(body, out_shape, operands, scalars=0, scratch=(), flops=0, limit=16, outside=(), resident=(), out_space=pltpu.VMEM):
    specs = [pl.BlockSpec(memory_space=pltpu.SMEM)] * scalars
    specs += [
        pl.BlockSpec(memory_space=pl.ANY if any(x is o for o in outside) else pltpu.VMEM) for x in operands[scalars:]
    ]
    many = isinstance(out_shape, (list, tuple))
    shapes = [pltpu.HBM(x.shape, x.dtype) for x in (out_shape if many else [out_shape])]
    out_specs = [pl.BlockSpec(memory_space=out_space)] * len(shapes)
    return pl.pallas_call(
        body,
        out_shape=shapes if many else shapes[0],
        in_specs=specs,
        out_specs=out_specs if many else out_specs[0],
        scratch_shapes=list(scratch),
        compiler_params=pltpu.CompilerParams(vmem_limit_bytes=limit * 1024 * 1024),
        cost_estimate=pl.CostEstimate(flops=flops, transcendentals=0, bytes_accessed=1 << 20),
    )(
        *[
            pltpu.with_memory_space_constraint(x, pltpu.VMEM) if any(x is r for r in resident) else in_hbm(x)
            for x in operands
        ]
    )


class Arrival:
    def __init__(self, sources, target, arrived):
        self.copies = [pltpu.make_async_copy(ref, target.at[i], arrived.at[i]) for i, ref in enumerate(sources)]
        for copy in self.copies:
            copy.start()

    def wait(self, index):
        self.copies[index].wait()


def dot_nn(left, right):
    return lax.dot_general(left, right, (((1,), (0,)), ((), ())), preferred_element_type=F32)


def column_norm(values):
    return values * lax.rsqrt(jnp.mean(values * values, axis=0, keepdims=True) + NORM_EPSILON)


def exchanged(shard, axis, groups):
    return lax.all_to_all(shard, axis, 0, 0, axis_index_groups=groups)


def staged(weights):
    def body(*refs):
        out, arrived = refs[-2:]
        arrival = Arrival(refs[:-2], out, arrived)
        for index in range(len(weights)):
            arrival.wait(index)

    return pl.pallas_call(
        body,
        out_shape=pltpu.VMEM((len(weights), *weights[0].shape), weights[0].dtype),
        in_specs=[pl.BlockSpec(memory_space=pl.ANY)] * len(weights),
        out_specs=pl.BlockSpec(memory_space=pltpu.VMEM),
        scratch_shapes=[pltpu.SemaphoreType.DMA((len(weights),))],
        compiler_params=pltpu.CompilerParams(vmem_limit_bytes=8 * 1024 * 1024),
        name="staged",
    )(*[in_hbm(w) for w in weights])


def project(ids, pieces, squares, head_weights, conv_weights, gains, earlier, head_dim, slot_step, split, heads, conv):
    rows, features = pieces[0].shape
    _, width, attn_width = head_weights.shape
    channels = conv_weights[0].shape[1]
    head_count = attn_width // head_dim
    count = len(pieces)
    tail = min(128, rows)
    before = 0 if earlier is None else earlier.shape[2]
    earlier_list = [] if earlier is None else [earlier]
    pair_count = head_count if split else 1

    def body(ids_ref, *refs):
        piece_refs, refs = refs[:count], refs[count:]
        squares_ref, head_ref, refs = refs[0], refs[1], refs[2:]
        conv_refs, refs = refs[:3], refs[3:]
        query_gain_ref, key_gain_ref, refs = refs[0], refs[1], refs[2:]
        earlier_refs, refs = refs[: len(earlier_list)], refs[len(earlier_list) :]
        if heads:
            query_out, pair_outs, refs = refs[0], refs[1 : 1 + pair_count], refs[1 + pair_count :]
        if conv:
            outer_out, gated_out, tail_out = refs[:3]
            refs = refs[3:]
        held, product, weight_store, joined, arrived = refs
        copies = []
        for place, (offset, piece_ref) in enumerate(zip(xor_offsets(count), piece_refs)):
            start = pl.multiple_of((ids_ref[1] ^ offset) * features, features)
            copies.append(pltpu.make_async_copy(piece_ref, held.at[:, pl.ds(start, features)], joined.at[place]))
            copies[-1].start()
        if conv:
            arrival = Arrival(conv_refs, weight_store, arrived)
        row_scale = lax.rsqrt(squares_ref[...] / width + NORM_EPSILON)
        if heads and before:
            query_out[:, :, :before] = earlier_refs[0][...]
        own_slot = ids_ref[0] // slot_step
        for copy in copies:
            copy.wait()
        for index in range(3 if heads else 0):
            product[index] = dot_nn(held[...], head_ref[index]).T * row_scale
            for head in range(head_count):
                base = head * head_dim
                if split and index:
                    base = pl.multiple_of((own_slot ^ head) * head_dim, head_dim)
                part = product[index, pl.ds(base, head_dim), :]
                if index == 0:
                    query_out[head, :, before:] = (column_norm(part) * query_gain_ref[...]).astype(BF16)
                    continue
                settled = (column_norm(part) * key_gain_ref[...] if index == 1 else part).astype(BF16)
                span = slice((index - 1) * head_dim, index * head_dim)
                if split:
                    pair_outs[head][span, :] = settled
                else:
                    pair_outs[0][head, span, :] = settled
        if not conv:
            return
        for index in range(3):
            arrival.wait(index)
        outer_out[...] = dot_nn(held[...], weight_store[0]).T * row_scale
        inner = dot_nn(held[...], weight_store[1]).T * row_scale
        gated = (inner * (dot_nn(held[...], weight_store[2]).T * row_scale)).astype(BF16)
        gated_out[...] = gated
        tail_out[...] = gated[:, rows - tail :]

    head_shape = [jax.ShapeDtypeStruct((head_count, head_dim, before + rows), BF16)]
    if split:
        head_shape += [jax.ShapeDtypeStruct((2 * head_dim, rows), BF16)] * head_count
    else:
        head_shape += [jax.ShapeDtypeStruct((head_count, 2 * head_dim, rows), BF16)]
    conv_shape = [
        jax.ShapeDtypeStruct((channels, rows), F32),
        jax.ShapeDtypeStruct((channels, rows), BF16),
        jax.ShapeDtypeStruct((channels, tail), BF16),
    ]
    outs = vmem_call(
        body,
        (head_shape if heads else []) + (conv_shape if conv else []),
        [ids, *pieces, squares, head_weights, *conv_weights, *gains, *earlier_list],
        scalars=1,
        scratch=[
            pltpu.VMEM((rows, width), BF16),
            pltpu.VMEM((3, attn_width, rows), F32),
            pltpu.VMEM((3, width, channels), BF16),
            pltpu.SemaphoreType.DMA((count,)),
            pltpu.SemaphoreType.DMA((3,)),
        ],
        flops=2 * 3 * (attn_width + channels) * rows * width,
        limit=28,
        outside=(*conv_weights, *pieces) if heads else (*conv_weights, *pieces, head_weights),
        resident=(head_weights,) if heads else (),
    )
    return outs


def finish_conv(ids, outers, gateds, prior, taps, gain, group, tile_count):
    channels, chunk_rows = gateds[0].shape
    count = len(gateds)
    rows = chunk_rows * count
    tail = prior.shape[1]
    tap_count = taps.shape[1]
    tile_rows = rows // tile_count

    def body(ids_ref, *refs):
        outer_refs, gated_refs = refs[:count], refs[count : 2 * count]
        prior_ref, taps_ref, gain_ref = refs[2 * count : 2 * count + 3]
        outs, out = refs[2 * count + 3 : -1], refs[-1]
        lane = lax.broadcasted_iota(jnp.int32, (group, tail), 1)
        for index in range(channels // group):
            span = slice(index * group, (index + 1) * group)
            values = jnp.concatenate([ref[span, :].astype(F32) for ref in gated_refs], axis=1)
            outer = jnp.concatenate([ref[span, :] for ref in outer_refs], axis=1)
            before = prior_ref[span, :].astype(F32)
            weights = taps_ref[span, :]
            total = weights[:, tap_count - 1 : tap_count] * values
            for back in range(1, tap_count):
                moved = pltpu.roll(values, back, 1)
                head = jnp.where(lane < back, pltpu.roll(before, back, 1), moved[:, :tail])
                moved = jnp.concatenate([head, moved[:, tail:]], axis=1)
                total = total + weights[:, tap_count - 1 - back : tap_count - back] * moved
            mixed = (column_norm(outer * total) * gain_ref[span, :]).astype(BF16)
            for tile in range(tile_count):
                out[tile, span, :] = mixed[:, tile * tile_rows : (tile + 1) * tile_rows]
        for ref, offset in zip(outs, xor_offsets(tile_count)):
            ref[...] = out[ids_ref[1] ^ offset]

    return vmem_call(
        body,
        [jax.ShapeDtypeStruct((channels, tile_rows), BF16)] * tile_count,
        [ids, *outers, *gateds, prior, taps, gain],
        scalars=1,
        scratch=[pltpu.VMEM((tile_count, channels, tile_rows), BF16)],
        flops=1 << 20,
    )


def attend(ids, queries, pairs, gates, gain, lane_count, tile_count):
    chunk_count = len(pairs[0])
    slot_count, head_dim, rows = queries.shape
    counts = [len(chunk) for chunk in pairs[0]]
    flat_pairs = [kv for lane in pairs for chunk in lane for kv in chunk]
    chunk_rows = rows // chunk_count
    tile_rows = rows // tile_count
    q_tile = min(QUERY_TILE, chunk_rows)
    k_tile = q_tile
    q_tiles = rows // q_tile
    per_chunk = chunk_rows // k_tile
    block_count = slot_count * lane_count
    steps = slot_count * q_tiles
    wide = 2 * head_dim
    exponent_scale = LOG2_E * float(head_dim) ** -0.5
    subtiles = q_tile // tile_rows
    blocks = [slot * lane_count + (lane_count - 1 if slot % 2 else 0) for slot in range(slot_count)]
    full_tiles = sum(block * q_tiles + part for block in blocks for part in range(q_tiles))
    unroll = next(n for n in (4, 2, 1) if full_tiles % n == 0)

    def body(ids_ref, *refs):
        query_ref, refs = refs[0], refs[1:]
        flat_refs, refs = refs[: len(flat_pairs)], refs[len(flat_pairs) :]
        gate_refs, refs = refs[:lane_count], refs[lane_count:]
        gain_ref, out, key_store, value_store, query_store, score_store = refs[:6]
        top_store, total_store, arrived = refs[6:9]
        stages = refs[9:]
        copies = [pltpu.make_async_copy(ref, stage, arrived.at[i]) for i, (ref, stage) in enumerate(zip(flat_refs, stages))]
        for copy in copies:
            copy.start()
        own = ids_ref[0]
        own_slot = own // lane_count
        own_lane = own % lane_count
        query_lane = jnp.where(own_slot % 2 == 0, own_lane, lane_count - 1 - own_lane)

        ones = (lax.broadcasted_iota(jnp.int32, (head_dim, q_tile), 0) < 3).astype(F32).astype(BF16)
        for slot in range(slot_count):
            for part in range(q_tiles):
                index = slot * q_tiles + part
                query = query_ref[slot, :, part * q_tile : (part + 1) * q_tile].astype(F32) * exponent_scale
                coarse = query.astype(BF16)
                query_store[index, 0:head_dim, :] = coarse
                query_store[index, head_dim:wide, :] = ones
                query_store[index, wide : wide + head_dim, :] = (query - coarse.astype(F32)).astype(BF16)
                query_store[index, wide + head_dim : 2 * wide, :] = jnp.zeros_like(coarse)

        row8 = lax.broadcasted_iota(jnp.int32, (8, k_tile), 0)
        filler = jnp.zeros((head_dim - 8, k_tile), F32)

        def settle(ref, slot, lane, chunk):
            block = slot * lane_count + (own_lane ^ lane)
            for part in range(per_chunk):
                span = slice(part * k_tile, (part + 1) * k_tile)
                at = chunk * chunk_rows + part * k_tile
                index = block * q_tiles + chunk * per_chunk + part
                gate = gate_refs[lane][pl.ds(slot, 1), at : at + k_tile] * (-LOG2_E)
                first = gate.astype(BF16).astype(F32)
                rest = gate - first
                second = rest.astype(BF16).astype(F32)
                third = rest - second
                gate_rows = jnp.where(row8 == 0, first, jnp.where(row8 == 1, second, jnp.where(row8 == 2, third, 0.0)))
                stacked = jnp.concatenate([ref[0:head_dim, span].astype(F32), gate_rows, filler], axis=0)
                key_store[index] = stacked.T.astype(BF16)
                value_store[index] = ref[head_dim:wide, span]

        cursor = 0
        for lane in range(lane_count):
            for chunk in range(chunk_count):
                for member in range(counts[chunk]):
                    copies[cursor].wait()
                    if counts[chunk] > 1:
                        settle(stages[cursor], own_slot ^ member, lane, chunk)
                    else:
                        for slot in range(slot_count):
                            settle(stages[cursor].at[slot], slot, lane, chunk)
                    cursor += 1

        def tile_of(step):
            slot = step // q_tiles
            block = slot * lane_count + jnp.where(slot % 2 == 0, query_lane, lane_count - 1 - query_lane)
            return block * q_tiles + step % q_tiles

        def score(step, tile, place, masked):
            keys = key_store[tile]
            scores = dot_nn(jnp.concatenate([keys, keys], axis=1), query_store[step])
            if masked:
                key_at = lax.broadcasted_iota(jnp.int32, (k_tile, q_tile), 0)
                query_at = lax.broadcasted_iota(jnp.int32, (k_tile, q_tile), 1)
                scores = jnp.where(key_at <= query_at, scores, -1e30)
            score_store[place] = scores
            highest = jnp.max(scores, axis=0, keepdims=True)
            if masked:
                top_store[step] = highest
                return highest, None
            old = top_store[step]
            top = jnp.maximum(old, highest)
            top_store[step] = top
            return top, jnp.exp2(old - top)

        def absorb(step, tile, place, top, factor):
            weights = jnp.exp2(score_store[place] - top).astype(BF16)
            added = dot_nn(value_store[tile], weights)
            total_store[step] = added if factor is None else total_store[step] * factor + added

        top, _ = score(0, tile_of(0), 0, True)

        def on_diagonal(pair, top):
            step = 2 * pair
            middle, _ = score(step + 1, tile_of(step + 1), 1, True)
            absorb(step, tile_of(step), 0, top, None)
            following = jnp.minimum(step + 2, steps - 1)
            latest, _ = score(following, tile_of(following), 0, True)
            absorb(step + 1, tile_of(step + 1), 1, middle, None)
            return latest

        lax.fori_loop(0, steps // 2, on_diagonal, top)

        def following(step, tile):
            done = tile + 1 >= tile_of(step)
            return jnp.where(done, jnp.minimum(step + 1, steps - 1), step), jnp.where(done, 0, tile + 1)

        step = jnp.where(tile_of(0) == 0, 1, 0)
        top, factor = score(step, 0, 0, False)

        def below(turn, carry):
            step, tile, top, factor = carry
            for count in range(unroll):
                next_step, next_tile = following(step, tile)
                place = count % 2
                if unroll == 1:
                    absorb(step, tile, 0, top, factor)
                    next_top, next_factor = score(next_step, next_tile, 0, False)
                elif count < unroll - 1:
                    next_top, next_factor = score(next_step, next_tile, 1 - place, False)
                    absorb(step, tile, place, top, factor)
                else:
                    more = turn + 1 < full_tiles // unroll
                    next_step = jnp.where(more, next_step, step)
                    next_tile = jnp.where(more, next_tile, tile)
                    next_top, next_factor = score(next_step, next_tile, 0, False)
                    absorb(step, tile, 1, top, factor)
                step, tile, top, factor = next_step, next_tile, next_top, next_factor
            return step, tile, top, factor

        lax.fori_loop(0, full_tiles // unroll, below, (step, jnp.int32(0), top, factor))

        head_gain = gain_ref[own_slot]
        for step in range(steps):
            mixed = (column_norm(total_store[step]) * head_gain).astype(BF16)
            for sub in range(subtiles):
                out[step * subtiles + sub] = mixed[:, sub * tile_rows : (sub + 1) * tile_rows]

    return vmem_call(
        body,
        jax.ShapeDtypeStruct((slot_count * tile_count, head_dim, tile_rows), BF16),
        [ids, queries, *flat_pairs, *gates, gain],
        scalars=1,
        scratch=[
            pltpu.VMEM((block_count * q_tiles, k_tile, wide), BF16),
            pltpu.VMEM((block_count * q_tiles, head_dim, k_tile), BF16),
            pltpu.VMEM((steps, 2 * wide, q_tile), BF16),
            pltpu.VMEM((2, k_tile, q_tile), F32),
            pltpu.VMEM((steps, 1, q_tile), F32),
            pltpu.VMEM((steps, head_dim, q_tile), F32),
            pltpu.SemaphoreType.DMA((len(flat_pairs),)),
            *[pltpu.VMEM(kv.shape, BF16) for kv in flat_pairs],
        ],
        flops=4 * head_dim * slot_count * rows * block_count * rows,
        limit=28,
        outside=flat_pairs,
    )


def output_rows(ids, pieces, weights, base, early=None):
    source_count = len(weights)
    early_count = 0 if early is None else early.shape[0]
    early_list = [early] if early_count else []
    weights = weights[early_count:]
    listed = isinstance(pieces, (list, tuple))
    piece_list = list(pieces) if listed else [pieces]
    piece_count, piece_height, rows = (len(pieces), *pieces[0].shape) if listed else pieces.shape
    slot_count = piece_count // source_count
    height = slot_count * piece_height
    width = weights[0].shape[1]
    offsets = xor_offsets(source_count)
    bases = [] if base is None else [base]
    parts = OUTPUT_PARTS
    part_width = width // parts

    def body(ids_ref, *refs):
        piece_refs, refs = refs[: len(piece_list)], refs[len(piece_list) :]
        early_refs, refs = refs[: len(early_list)], refs[len(early_list) :]
        weight_refs, refs = refs[: len(weights)], refs[len(weights) :]
        base_refs, refs = refs[: len(bases)], refs[len(bases) :]
        out_ref, held, weight_store, result, joined, arrived, left = refs[:7]
        gathers = []
        for place, offset in enumerate(offsets):
            source = ids_ref[1] ^ offset
            for slot in range(slot_count):
                start = place * height + slot * piece_height
                gathers.append(
                    pltpu.make_async_copy(
                        piece_refs[place] if listed else piece_refs[0].at[slot * source_count + source],
                        held.at[start : start + piece_height, :],
                        joined.at[place * slot_count + slot],
                    )
                )
                gathers[-1].start()
        arrival = Arrival(weight_refs, weight_store, arrived)
        if bases:
            below = pltpu.make_async_copy(base_refs[0], refs[7], refs[8].at[0])
            below.start()
        for copy in gathers:
            copy.wait()
        turned = held[...].T
        for place in range(len(weights)):
            arrival.wait(place)
        if bases:
            below.wait()
        stores = []
        for part in range(parts):
            span = slice(part * part_width, (part + 1) * part_width)
            slices = [early_refs[0][place, :, span] for place in range(early_count)]
            slices += [weight_store[place, :, span] for place in range(len(weights))]
            weight = jnp.concatenate(slices, axis=0)
            total = dot_nn(turned, weight)
            if bases:
                total = total + refs[7][:, span].astype(F32)
            result[:, span] = total.astype(BF16)
            stores.append(pltpu.make_async_copy(result.at[:, span], out_ref.at[:, span], left.at[part]))
            stores[-1].start()
        for copy in stores:
            copy.wait()

    scratch = [
        pltpu.VMEM((source_count * height, rows), BF16),
        pltpu.VMEM((len(weights), height, width), BF16),
        pltpu.VMEM((rows, width), BF16),
        pltpu.SemaphoreType.DMA((piece_count,)),
        pltpu.SemaphoreType.DMA((len(weights),)),
        pltpu.SemaphoreType.DMA((parts,)),
    ]
    if bases:
        scratch += [pltpu.VMEM((rows, width), BF16), pltpu.SemaphoreType.DMA((1,))]
    return vmem_call(
        body,
        jax.ShapeDtypeStruct((rows, width), BF16),
        [ids, *piece_list, *early_list, *weights, *bases],
        scalars=1,
        scratch=scratch,
        flops=2 * source_count * height * rows * width,
        outside=(*piece_list, *weights, *bases),
        resident=early_list,
        out_space=pl.ANY,
    )


def per_device(
    tokens,
    mix_gain,
    query_weight,
    key_weight,
    value_weight,
    outer_gate_weight,
    inner_gate_weight,
    conv_input_weight,
    query_gain,
    key_gain,
    gate_totals,
    conv_taps,
    attn_out_gain,
    conv_out_gain,
    attn_out_weight,
    conv_out_weight,
):
    rows, features = tokens.shape
    head_dim = query_gain.shape[0]
    head_count = query_weight.shape[1] // head_dim
    sp_count = lax.axis_size("sp")
    tp_count = lax.axis_size("tp")
    lane_count = sp_count // head_count
    sp_index = lax.axis_index("sp")
    tp_index = lax.axis_index("tp")
    ids = jnp.stack([sp_index, tp_index]).astype(jnp.int32)
    chunk_rows = rows // ROW_CHUNKS
    straight = [[slot * lane_count + lane for slot in range(head_count)] for lane in range(lane_count)]
    snaked = [
        [slot * lane_count + (lane_count - 1 - lane if slot % 2 else lane) for slot in range(head_count)]
        for lane in range(lane_count)
    ]
    snaked_wide = [[p * tp_count + t for p in group for t in range(tp_count)] for group in snaked]

    own_gain = lax.dynamic_slice_in_dim(mix_gain, tp_index * features, features, 0)
    scaled = [
        (tokens[c * chunk_rows : (c + 1) * chunk_rows].astype(F32) * own_gain).astype(BF16) for c in range(ROW_CHUNKS)
    ]
    far = []
    for c in range(ROW_CHUNKS):
        far.append(swapped(scaled[c], "tp", tp_count >> 1))
    tokens, gate_totals = lax.optimization_barrier((tokens, gate_totals, *scaled))[:2]
    widened = tokens.astype(F32)
    squares = jnp.sum(widened * widened, axis=1).reshape(1, rows)
    gains = (query_gain.reshape(-1, 1), key_gain.reshape(-1, 1))
    out_gains = (attn_out_gain.reshape(head_count, head_dim, 1), conv_out_gain.reshape(-1, 1), conv_taps.T)
    slot_gates = exchanged(gate_totals.T, "sp", straight)
    gates = [slot_gates] + [swapped(slot_gates, "sp", lane) for lane in range(1, lane_count)]
    attn_weight = staged((query_weight, key_weight, value_weight))
    conv_weight = (outer_gate_weight, inner_gate_weight, conv_input_weight)
    squares, ids, gains, out_gains, gates, attn_weight = lax.optimization_barrier(
        (squares, ids, gains, out_gains, gates, attn_weight)
    )
    bit = tp_count >> 1
    while bit:
        squares = squares + swapped(squares, "tp", bit)
        bit >>= 1
    chunks = []
    for c in range(ROW_CHUNKS):
        pieces = [scaled[c], far[c]]
        bit = tp_count >> 2
        while bit:
            pieces = pieces + [swapped(piece, "tp", bit) for piece in pieces]
            bit >>= 1
        chunks.append(pieces)

    queries, conv_outs = None, [None] * ROW_CHUNKS
    pairs = [[] for _ in range(lane_count)]
    for c in range(ROW_CHUNKS):
        chunk_squares = squares[:, c * chunk_rows : (c + 1) * chunk_rows]
        split = c > 0
        shared = (ids, chunks[c], chunk_squares, attn_weight, conv_weight, gains, queries, head_dim, lane_count, split)
        outs = project(*shared, True, split)
        queries, own_pairs = outs[0], outs[1 : 1 + (head_count if split else 1)]
        if split:
            conv_outs[c] = outs[-3:]
        if split:
            moved = [swapped(p, "sp", i * lane_count) if i else p for i, p in enumerate(own_pairs)]
        else:
            moved = [exchanged(own_pairs[0], "sp", straight)]
        pairs[0].append(moved)
        for lane in range(1, lane_count):
            through = []
            for p in moved:
                through.append(swapped(p, "sp", lane))
            pairs[lane].append(through)
    conv_outs[0] = project(
        ids, chunks[0], squares[:, :chunk_rows], attn_weight, conv_weight, gains, None, head_dim, lane_count, False, False, True
    )
    outers, gateds = [o[0] for o in conv_outs], [o[1] for o in conv_outs]
    prior = lax.ppermute(conv_outs[-1][2], "sp", [(i, i + 1) for i in range(sp_count - 1)])
    queries = exchanged(queries, "sp", snaked)

    far_weights = lax.optimization_barrier((attn_out_weight, conv_out_weight, far[-1]))[:2]
    half = tp_count >> 1
    far_weights = [swapped(weight, "tp", half) for weight in far_weights]

    conv_mixed = finish_conv(
        ids, outers, gateds, prior, out_gains[2], out_gains[1], head_dim, tp_count
    )
    conv_pieces = [
        swapped(piece, "tp", offset) if offset else piece
        for piece, offset in zip(conv_mixed, xor_offsets(tp_count))
    ]
    attended = attend(
        ids, queries, pairs, gates, out_gains[0], lane_count, tp_count
    )
    attn_pieces = lax.all_to_all(attended, ("sp", "tp"), 0, 0, axis_index_groups=snaked_wide)
    own_weights = lax.optimization_barrier((attn_out_weight, conv_out_weight, *far_weights, attended))[:4]
    gathered = []
    for own, distant in zip(own_weights[:2], own_weights[2:]):
        parts = [own, distant]
        bit = tp_count >> 2
        while bit:
            parts = parts + [swapped(part, "tp", bit) for part in parts]
            bit >>= 1
        gathered.append(parts)
    base = output_rows(ids, conv_pieces, gathered[1], None)
    early = staged(gathered[0][: tp_count // 2])
    return output_rows(ids, attn_pieces, gathered[0], base, early)


def solution(mesh):
    placed = (
        P("sp", "tp"),
        P(),
        P(None, "tp"),
        P(None, "tp"),
        P(None, "tp"),
        P(None, "tp"),
        P(None, "tp"),
        P(None, "tp"),
        P(),
        P(),
        P("sp", "tp"),
        P(None, "tp"),
        P("tp"),
        P("tp"),
        P("tp", None),
        P("tp", None),
    )
    return jax.shard_map(per_device, mesh=mesh, in_specs=placed, out_specs=P(("sp", "tp"), None), check_vma=False)
```
